512 devices in a mesh: ep: 32 (over z, x), tp: 16 (over y, core).
Axes of the slice: x: 4, y: 8, z: 8, core: 2. Of those that a mesh axis runs over, the one named last changes fastest.
Arguments:
- tokens: bfloat16 [4096, 4096], P('ep', 'tp'), may hold values from -6 to 6
- cotangent: bfloat16 [4096, 4096], P('ep', 'tp'), may hold values from -6 to 6
- routes: int32 [4096, 2], P('ep'), may hold values from 0 to 31, all different within a row; in each aligned block of 128 rows (0 to 127, 128 to 255, ...) at most 12 rows name the same one
- gate_weight: float32 [4096, 2], P('ep'), may hold values from 0.1 to 2.5
- w_gate: bfloat16 [32, 1024, 4096], P('ep', 'tp'), may hold values from -0.09375 to 0.09375
- w_up: bfloat16 [32, 1024, 4096], P('ep', 'tp'), may hold values from -0.09375 to 0.09375
- w_down: bfloat16 [32, 1024, 4096], P('ep', 'tp'), may hold values from -0.1875 to 0.1875
- shared_hidden: bfloat16 [4096, 1024], P('ep'), may hold values from -4 to 4
Outputs:
- tokens_grad: bfloat16 [4096, 4096], P('ep', 'tp')
- gate_grad: float32 [4096, 2], P('ep')
- w_gate_grad: float32 [32, 1024, 4096], P('ep', 'tp')
- w_up_grad: float32 [32, 1024, 4096], P('ep', 'tp')
- w_down_grad: float32 [32, 1024, 4096], P('ep', 'tp')
- shared_grad: float32 [1024, 4096], P('ep', 'tp')
The draws below stay inside these ranges and needn't reach their ends.
Inputs may be any that keep to these rules, and one draw needn't show every extreme that they name: `routes`: each row names 2 different experts. Among the rows of one index of ep (aligned blocks of 128 rows) no expert is named more than 12 times, and in every draw some expert is named exactly 12 times in some block.
All inputs are finite; a program needn't handle non-finite values.
Results may differ from the reference program's by a relative error of at most 0.022.
Values may be sent and summed in bfloat16 or wider, within the bound.
A program may use at most 64 MiB of HBM per device.

```python
import math
import jax
import jax.numpy as jnp
import numpy as np
from jax import lax

D = 4096
HIDDEN_SIZE = 1024
SHARED_HIDDEN = 1024
TOP_K = 2
TOK_DEV = 128
EXPERTS = 32
CAP = 12
TOKENS = 4096
N_EP = 32
N_TP = 16


def with_spikes(drawn, rng, source, target, parts, factor):
    def block_of(position):
        return (jnp.arange(drawn.shape[position]) // (drawn.shape[position] // parts)).reshape((-1,) + (1,) * (drawn.ndim - 1 - position))

    near = jax.random.permutation(rng, parts)[block_of(target)]
    second = (block_of(target) + parts // 2) % parts
    return jnp.where((block_of(source) == near) | (block_of(source) == second), factor * drawn, drawn)


def levels(rng, shape, pieces, low, largest):
    def one(axis_at, shards_of):
        heights = jax.random.uniform(jax.random.fold_in(jax.random.fold_in(rng, 6), axis_at), (shards_of,), jnp.float32, low / len(pieces), largest / len(pieces))
        return jnp.repeat(jnp.exp(heights), shape[axis_at] // shards_of).reshape((-1,) + (1,) * (len(shape) - axis_at - 1))

    level = one(*pieces[0])
    for cut in pieces[1:]:
        level = level * one(*cut)
    return level


def deal_out(rng, own, number, rows, count, top, bound, lean):
    ranking = jax.random.permutation(rng, count)
    packed, common = portions_of(count, rows * top, bound, lean, True), portions_of(count, rows * top, bound, lean, False)
    places = jnp.arange(count)

    def named(tallies, turn):
        used = int((tallies > 0).sum())
        fixed = max(1, used // 4)
        moved = fixed + (places - fixed + turn * (used - fixed)) % max(1, count - fixed)
        return jnp.zeros((count,), jnp.int32).at[ranking[jnp.where(places < fixed, places, moved)]].set(jnp.asarray(tallies, jnp.int32))

    tallies = jnp.where(number % 4 == 0, named(packed, number // 4), named(common, number - number // 4 - 1))
    mixed = jax.random.permutation(jax.random.fold_in(own, 3), count)
    giver, receiver = mixed[0:count // 2 * 2:2], mixed[1:count // 2 * 2:2]
    room = jnp.minimum(tallies[giver] - 1, bound - tallies[receiver]) // 2
    room = jnp.where((giver == ranking[0]) | (receiver == ranking[0]) | (tallies[receiver] == 0), 0, jnp.maximum(room, 0))
    moved = jax.random.randint(jax.random.fold_in(own, 4), (count // 2,), 0, 1 << 20) % (room + 1)
    tallies = tallies.at[giver].add(-moved).at[receiver].add(moved)
    items = jnp.searchsorted(jnp.cumsum(tallies), jnp.arange(rows * top), side="right").astype(jnp.int32)
    table = items.reshape(top, rows).T
    table = table[jax.random.permutation(jax.random.fold_in(own, 1), rows)]
    turn = jax.random.randint(jax.random.fold_in(own, 2), (rows, 1), 0, top)
    return jnp.take_along_axis(table, (jnp.arange(top)[None, :] + turn) % top, axis=1)


def portions_of(count, total, limit, slope, full):
    portions = [(1 << 20) // math.isqrt(grade ** slope) + 1 for grade in range(1, count + 1)]
    largest = limit if full else min(limit, max(-(-total // count), total * portions[0] // sum(portions)))
    least = 1 if total - largest >= count - 1 else 0
    holding, surplus = [largest] + [least] * (count - 1), total - largest - least * (count - 1)
    while surplus > 0:
        movable = [i for i in range(1, count) if holding[i] < largest] or [i for i in range(1, count) if holding[i] < limit]
        whole, left = sum([portions[i] for i in movable]), surplus
        for i in movable:
            extra = min(limit - holding[i], max(1, left * portions[i] // whole), surplus)
            holding[i] = holding[i] + extra
            surplus = surplus - extra
    return np.array(holding)


def centred(key, dims, spread, bound, split=(), kind=jnp.bfloat16):
    drawn = spread * jax.random.normal(key, dims, jnp.float32)
    if split:
        drawn = drawn * levels(key, dims, split, -0.22, 0.18)
    return jnp.clip(drawn, -bound, bound).astype(kind)


def bell_draw_with(stream_key, extent, spread, most, cuts, heavy, kind=jnp.bfloat16):
    drawn = spread * jax.random.normal(stream_key, extent, jnp.float32)
    if cuts:
        drawn = drawn * levels(stream_key, extent, cuts, -0.22, 0.18)
    return jnp.clip(with_spikes(drawn, jax.random.fold_in(stream_key, 3), *heavy), -most, most).astype(kind)


def setup_inputs(seed: int = 0) -> dict:
    key_list = jax.random.split(jax.random.key(seed), 9)
    tokens = centred(key_list[0], (TOKENS, D), 1.0, 6.0, ((0, 32), (1, 16)))
    cotangent = centred(key_list[1], (TOKENS, D), 1.0, 6.0, ((0, 32), (1, 16)))
    routes_keys = jax.random.split(jax.random.fold_in(key_list[2], 1), TOKENS // TOK_DEV)
    routes_turns = jax.random.permutation(jax.random.fold_in(key_list[2], 3), TOKENS // TOK_DEV)
    routes = jax.vmap(lambda own, number: deal_out(jax.random.fold_in(key_list[2], 2), own, number, TOK_DEV, EXPERTS, TOP_K, CAP, 2))(routes_keys, routes_turns).reshape((TOKENS, TOP_K))
    gate_weight = jnp.clip(jnp.exp(math.log(2.5) - 3.218876 * jax.random.uniform(key_list[3], (TOKENS, TOP_K), jnp.float32) ** levels(key_list[3], (TOKENS, TOP_K), ((0, 32),), -0.2, 0.2)), 0.1, 2.5)
    w_gate = centred(key_list[4], (EXPERTS, HIDDEN_SIZE, D), D ** -0.5, 0.09375, ((0, 32), (1, 16)))
    w_up = centred(key_list[5], (EXPERTS, HIDDEN_SIZE, D), D ** -0.5, 0.09375, ((0, 32), (1, 16)))
    w_down = centred(key_list[6], (EXPERTS, HIDDEN_SIZE, D), HIDDEN_SIZE ** -0.5, 0.1875, ((0, 32), (1, 16)))
    shared_hidden = bell_draw_with(key_list[7], (TOKENS, SHARED_HIDDEN), 0.5, 4.0, ((0, 32),), (0, 1, 32, 2.75))
    return {"tokens": tokens, "cotangent": cotangent, "routes": routes, "gate_weight": gate_weight, "w_gate": w_gate, "w_up": w_up, "w_down": w_down, "shared_hidden": shared_hidden}


def slot_positions(device_routes):
    flat_routes = device_routes.reshape(-1)
    onehot = (flat_routes[:, None] == jnp.arange(EXPERTS, dtype=jnp.int32)[None, :]).astype(jnp.int32)
    earlier = jnp.cumsum(onehot, axis=0) - onehot
    return flat_routes, jnp.sum(earlier * onehot, axis=1).astype(jnp.int32)


def reference(tokens, cotangent, routes, gate_weight, w_gate, w_up, w_down, shared_hidden):
    assigned = TOK_DEV * TOP_K
    flat_routes, positions = jax.vmap(slot_positions)(routes.reshape(N_EP, assigned))
    sources = jnp.broadcast_to(jnp.arange(N_EP, dtype=jnp.int32)[:, None], (N_EP, assigned))
    token_ids = sources * TOK_DEV + jnp.arange(assigned, dtype=jnp.int32)[None, :] // TOP_K
    slot_table = jnp.full((EXPERTS, N_EP, CAP), TOKENS, jnp.int32).at[flat_routes, sources, positions].set(token_ids)
    weight_table = jnp.zeros((EXPERTS, N_EP, CAP), jnp.float32).at[flat_routes, sources, positions].set(
        gate_weight.reshape(N_EP, assigned))
    padded_tokens = jnp.concatenate([tokens, jnp.zeros((1, D), jnp.bfloat16)], 0)
    padded_cotan = jnp.concatenate([cotangent, jnp.zeros((1, D), jnp.bfloat16)], 0)
    groups = HIDDEN_SIZE // N_TP
    contract_last = (((1,), (1,)), ((), ()))

    def expert_fn(inputs):
        table_rows, weight_rows, gate_mat, up_mat, down_mat = inputs
        rows_x = padded_tokens[table_rows.reshape(-1)]
        rows_g = padded_cotan[table_rows.reshape(-1)]
        weight_col = weight_rows.reshape(-1, 1)
        pre_gate = lax.dot_general(rows_x, gate_mat, contract_last, preferred_element_type=jnp.float32)
        pre_up = lax.dot_general(rows_x, up_mat, contract_last, preferred_element_type=jnp.float32)
        sigmoid_gate = jax.nn.sigmoid(pre_gate)
        silu_gate = pre_gate * sigmoid_gate
        hidden = (silu_gate * pre_up).astype(jnp.bfloat16)
        back_hidden = lax.dot_general(rows_g, down_mat, contract_last, preferred_element_type=jnp.float32)
        gate_part = jnp.sum(hidden.astype(jnp.float32) * back_hidden, axis=1)
        scaled = weight_col * back_hidden
        grad_pre_gate = (scaled * pre_up * sigmoid_gate * (1.0 + pre_gate * (1.0 - sigmoid_gate))).astype(jnp.bfloat16)
        grad_pre_up = (scaled * silu_gate).astype(jnp.bfloat16)
        weighted_cotan = (weight_col * rows_g.astype(jnp.float32)).astype(jnp.bfloat16)
        grad_down = jnp.dot(hidden.T, weighted_cotan, preferred_element_type=jnp.float32)
        grad_gate = jnp.dot(grad_pre_gate.T, rows_x, preferred_element_type=jnp.float32)
        grad_up = jnp.dot(grad_pre_up.T, rows_x, preferred_element_type=jnp.float32)
        row_total = rows_x.shape[0]
        partial_value = jnp.einsum('rnh,nhd->nrd', grad_pre_gate.astype(jnp.float32).reshape(row_total, N_TP, groups),
                             gate_mat.astype(jnp.float32).reshape(N_TP, groups, D))
        partial_value = partial_value + jnp.einsum('rnh,nhd->nrd', grad_pre_up.astype(jnp.float32).reshape(row_total, N_TP, groups),
                                       up_mat.astype(jnp.float32).reshape(N_TP, groups, D))
        rounded = lax.optimization_barrier(partial_value.astype(jnp.bfloat16)).astype(jnp.float32)
        row_grad = jnp.sum(rounded, axis=0).astype(jnp.bfloat16)
        return row_grad.reshape(N_EP, CAP, D), gate_part.reshape(N_EP, CAP), grad_gate, grad_up, grad_down

    row_grads, gate_parts, w_gate_grad, w_up_grad, w_down_grad = lax.map(
        expert_fn, (slot_table, weight_table, w_gate, w_up, w_down))
    picked = row_grads[flat_routes, sources, positions].astype(jnp.float32)
    tokens_grad = jnp.sum(picked.reshape(TOKENS, TOP_K, D), axis=1).astype(jnp.bfloat16)
    gate_grad = gate_parts[flat_routes, sources, positions].reshape(TOKENS, TOP_K)
    shared_grad = jnp.dot(shared_hidden.T, cotangent, preferred_element_type=jnp.float32)
    return (tokens_grad, gate_grad, w_gate_grad, w_up_grad, w_down_grad, shared_grad)
```

```python
import jax
import jax.numpy as jnp
import numpy as np
from jax import lax
from jax.experimental import pallas as pl
from jax.experimental.pallas import tpu as pltpu
from jax.sharding import PartitionSpec as P

MESH = pl.DeviceIdType.MESH
NZ, NX, NY = 8, 4, 8
NG = 4
ROWS = 16
BF = jnp.bfloat16
F32 = jnp.float32


def constants(blocks, cap):
    size = blocks // NG
    packed, gate_rows = size * cap, blocks // 2
    pack = np.zeros((packed, size * ROWS), np.float32)
    for q in range(size):
        for p in range(cap):
            pack[q * cap + p, q * ROWS + p] = 1
    spread = np.zeros((2, size * ROWS, size * ROWS), np.float32)
    for par in range(2):
        for q in range(size):
            for p in range(cap):
                spread[par, q * ROWS + p, gate_rows + q * cap + p] = 1
            spread[par, q * ROWS + cap, par * size + q] = 1
    total = blocks * cap
    owner = np.zeros((blocks, total), np.float32)
    place = np.zeros((total, 128), np.float32)
    for s in range(total):
        owner[s // cap, s] = 1
        place[s, s % cap] = 1
    return [jnp.asarray(a, BF) for a in (pack, spread)] + [
        jnp.asarray(owner, F32), jnp.asarray(place, BF)
    ]


def layer(cap, *refs):
    (tok, cot, routes, routes_t, gw, gw_t, shp, pack, spread, owner, place, wg, wu, wd) = refs[:14]
    (out_tok, out_gate, out_wg, out_wu, out_wd, out_sh) = refs[14:20]
    (w2, wdn, sx, sg, rx, rg, xg, shr, pre, back, gt, gn, ht, tile, ps, pr, srs, rrs) = refs[20:38]
    (fin, sb, rb, dgu, ddn, wsem, osem) = refs[38:45]
    (a2a_s, a2a_r, ag_s, ag_r, sib_s, sib_r, sh_s, sh_r) = refs[45:53]
    (pair_s, pair_r, rs_s, rs_r, rb_s, rb_r) = refs[53:]

    n_tok, feats = tok.shape
    blocks = NZ * NX
    size = blocks // NG
    vr, br, gate_rows = size * cap, size * ROWS, blocks // 2
    total = blocks * cap
    hop = NY // 2
    half = total // 2
    hid = wdn.shape[0]
    ep, tp = lax.axis_index("ep"), lax.axis_index("tp")
    z, x, y, c = ep // NX, ep % NX, tp // 2, tp % 2
    sibling = y * 2 + 1 - c

    def offset(r):
        q = r // NX
        odd = q % 2
        return (odd * ((q + 1) // 2) + (1 - odd) * (NZ - q // 2)) % NZ, r % NX

    def ahead(r):
        dz, dx = offset(r)
        return ((z + dz) % NZ) * NX + (x + dx) % NX

    def behind(r):
        dz, dx = offset(r)
        return ((z - dz + NZ) % NZ) * NX + (x - dx + NX) % NX

    def own_col(o):
        return ((y + o) % NY) * 2 + c

    def sib_col(o):
        return ((y + o) % NY) * 2 + 1 - c

    def arrived(ref, sem):
        pltpu.make_async_remote_copy(
            src_ref=ref, dst_ref=ref, send_sem=sem, recv_sem=sem,
            device_id=(ep, sibling), device_id_type=MESH,
        ).wait_recv()

    def send(src, dst, s_sem, r_sem, device):
        pltpu.make_async_remote_copy(
            src_ref=src, dst_ref=dst, send_sem=s_sem, recv_sem=r_sem,
            device_id=device, device_id_type=MESH,
        ).start()

    def dot(a, b):
        return jnp.dot(a, b, preferred_element_type=F32)

    def dot_nt(a, b):
        return lax.dot_general(a, b, (((1,), (1,)), ((), ())), preferred_element_type=F32)

    barrier = pltpu.get_barrier_semaphore()

    def greet(r, carry):
        pl.semaphore_signal(barrier, inc=1, device_id=(ahead(r), tp), device_id_type=MESH)
        return carry

    lax.fori_loop(1, blocks, greet, 0)
    for peer in (((y + 1) % NY) * 2 + c, ((y + NY - 1) % NY) * 2 + c, sibling):
        pl.semaphore_signal(barrier, inc=1, device_id=(ep, peer), device_id_type=MESH)

    loads = [
        pltpu.make_async_copy(wg.at[0], w2.at[pl.ds(0, hid)], wsem.at[0]),
        pltpu.make_async_copy(wu.at[0], w2.at[pl.ds(hid, hid)], wsem.at[1]),
        pltpu.make_async_copy(wd.at[0], wdn, wsem.at[2]),
    ]
    for load in loads:
        load.start()

    def rank_of(e):
        ez, ex = e // NX if NX & (NX - 1) else e >> (NX.bit_length() - 1), e & (NX - 1)
        dz, dx = (ez - z + NZ) & (NZ - 1), (ex - x + NX) & (NX - 1)
        q = jnp.where(dz <= NZ // 2, jnp.maximum(2 * dz - 1, 0), 2 * (NZ - dz))
        return (q * NX + dx).astype(F32)

    before = (
        lax.broadcasted_iota(jnp.int32, (n_tok, n_tok), 0)
        < lax.broadcasted_iota(jnp.int32, (n_tok, n_tok), 1)
    ).astype(F32)
    names = lax.broadcasted_iota(jnp.int32, (blocks, n_tok), 0)
    rows_e = [routes_t[k : k + 1, :] for k in range(2)]
    hot = [(names == e).astype(F32) for e in rows_e]
    seen = dot((hot[0] + hot[1]).astype(BF), before.astype(BF))
    slot_rows = [
        rank_of(rows_e[k]) * ROWS + jnp.sum(hot[k] * seen, axis=0, keepdims=True) for k in range(2)
    ]
    slots = lax.broadcasted_iota(jnp.int32, (blocks * ROWS, n_tok), 0).astype(F32)
    chosen = [(slots == d).astype(F32) for d in slot_rows]
    weight = jnp.sum(
        chosen[0] * gw_t[0:1, :] + chosen[1] * gw_t[1:2, :], axis=1, keepdims=True
    )
    table = (chosen[0] + chosen[1]).astype(BF)
    sx[...] = dot(table, tok[...]).astype(BF)
    sg[...] = (dot(table, cot[...]) * weight).astype(BF)
    rx[pl.ds(0, ROWS), :] = sx[pl.ds(0, ROWS), :]
    rg[pl.ds(0, ROWS), :] = sg[pl.ds(0, ROWS), :]

    pl.semaphore_wait(barrier, blocks - 1 + 3)

    for a, (src, dst) in enumerate(((sx, rx), (sg, rg))):
        for g in range(NG):

            def to_expert(r, carry, a=a, src=src, dst=dst, g=g):
                rows = pl.ds(pl.multiple_of(r * ROWS, ROWS), ROWS)
                send(src.at[rows], dst.at[rows], a2a_s.at[a], a2a_r.at[a, g], (ahead(r), tp))
                return carry

            lax.fori_loop(max(1, g * size), (g + 1) * size, to_expert, 0)

    def share(r, carry):
        e = ahead(r)
        n = out_sh.shape[0]
        rows = pl.ds(pl.multiple_of(e * n, n), n)
        send(shp.at[rows], shr.at[r], sh_s, sh_r, (e, tp))
        return carry

    def ring(a, way, h, k):
        d = 0 if way > 0 else 1
        part = xg.at[a, own_col(NY - h * way), pl.ds(k * half, half)]
        send(part, part, ag_s.at[a, d, h], ag_r.at[a, d, h, k], (ep, ((y + way + NY) % NY) * 2 + c))

    def to_sibling(a, o, k):
        part = xg.at[a, own_col(o), pl.ds(k * half, half)]
        send(part, part, sib_s.at[a], sib_r.at[a, o, k], (ep, sibling))

    for a, dst in enumerate((rx, rg)):
        for g in range(NG):
            lo = ROWS if g == 0 else 0
            arrived(dst.at[pl.ds(g * br + lo, br - lo)], a2a_r.at[a, g])
            got = dot(pack[...], dst[pl.ds(g * br, br), :])
            xg[a, own_col(0), pl.ds(g * vr, vr), :] = got.astype(BF)
            if g % 2 == 1:
                k = g // 2
                for way in (1, -1):
                    if hop > 1 or k == (0 if way > 0 else 1):
                        ring(a, way, 0, k)
                to_sibling(a, 0, k)
        if a == 1:
            lax.fori_loop(1, blocks, share, 0)

    for load in loads:
        load.wait()

    def forward(a, o, first=False):
        for k in range(2):
            arrived(xg.at[a, sib_col(o), pl.ds(k * half, half)], sib_r.at[a, o, k])
        acc, w = (pre, w2) if a == 0 else (back, wdn)
        part = None
        for j in (own_col(o), sib_col(o)):
            cols = pl.ds(pl.multiple_of(j * feats, feats), feats)
            term = dot_nt(w[:, cols], xg[a, j])
            part = term if part is None else part + term
        acc[...] = part if first else acc[...] + part

    for h in range(1, hop + 1):
        for a in range(2):
            for k in range(2):
                for d, way in enumerate((1, -1)):
                    if h == hop and k != d:
                        continue
                    o = (NY - h * way) % NY
                    part = xg.at[a, own_col(o), pl.ds(k * half, half)]
                    arrived(part, ag_r.at[a, d, h - 1, k])
                    if h < hop - 1 or (h == hop - 1 and k == d):
                        ring(a, way, h, k)
                    to_sibling(a, o, k)
        for a in range(2):
            if h == 1:
                forward(a, 0, first=True)
            else:
                forward(a, h - 1)
                forward(a, NY - h + 1)
    for a in range(2):
        forward(a, hop)

    s, u, b = pre[pl.ds(0, hid), :], pre[pl.ds(hid, hid), :], back[...]
    sig = 1.0 / (1.0 + jnp.exp(-s))
    silu = s * sig
    hidden = (silu * u).astype(BF)
    ht[...] = hidden
    grad_gate = b * u * sig * (1.0 + s * (1.0 - sig))
    grad_up = b * silu
    both = jnp.concatenate([grad_gate, grad_up], axis=0)
    gt[...] = both.astype(BF)
    gn[...] = both.T.astype(BF)
    gate_row = jnp.sum(hidden.astype(F32) * b, axis=0, keepdims=True)
    by_block = dot((owner[...] * gate_row).astype(BF), place[...])
    tile[...] = jnp.concatenate([by_block[:gate_rows], by_block[gate_rows:]], axis=1)

    def pair(o):
        cols = pl.ds(pl.multiple_of(sib_col(o) * feats, feats), feats)
        ps[o, pl.ds(0, gate_rows), :] = tile[...].astype(BF)
        ps[o, pl.ds(gate_rows, total), :] = dot(gn[...], w2[:, cols]).astype(BF)
        send(ps.at[o], pr.at[o], pair_s, pair_r.at[o], (ep, sibling))

    def rows_of(k):
        return pl.ds(0, gate_rows + vr) if k == 0 else pl.ds(gate_rows + k * vr, vr)

    def summed(o, k, others):
        cols = pl.ds(pl.multiple_of(own_col(o) * feats, feats), feats)
        mine = dot(gn[pl.ds(k * vr, vr), :], w2[:, cols])
        rest = pr[o, rows_of(k), :].astype(F32)
        for ref in others:
            rest = rest + ref[rows_of(k), :].astype(F32)
        if k > 0:
            return None, rest + mine
        return rest[:gate_rows] + tile[...], rest[gate_rows:] + mine

    def weights(j):
        cols = pl.ds(j * feats, feats)
        dgu[:, cols] = dot(gt[...], xg[0, j])
        ddn[:, cols] = dot(ht[...], xg[1, j])

    def rs_send(d, st, k):
        way = 1 - 2 * d
        part = pl.ds(*((0, gate_rows + vr) if k == 0 else (gate_rows + k * vr, vr)))
        send(
            srs.at[d, st, part], rrs.at[d, st, part], rs_s.at[d, st, k], rs_r.at[d, st, k],
            (ep, ((y + way + NY) % NY) * 2 + c),
        )

    started, todo = [], list(range(2 * NY))

    def some_weights(n):
        for _ in range(n):
            if todo:
                weights(todo.pop(0))

    pending = [hop] + [o for i in range(hop - 1, 0, -1) for o in (i, NY - i)] + [0]
    done = []

    def pairs_up_to(n):
        while len(done) < n:
            pair(pending[len(done)])
            done.append(1)

    ready = []

    def need(o):
        if o not in ready:
            arrived(pr.at[o], pair_r.at[o])
            ready.append(o)

    pairs_up_to(3)
    for st in range(hop):
        for k in range(NG):
            for d in range(2):
                mine = k // (NG // 2) == d
                if st == 0 and not mine:
                    continue
                way = 1 - 2 * d
                o = (way * (hop - st)) % NY
                need(o)
                others = []
                if st > 1 or (st == 1 and mine):
                    arrived(rrs.at[d, st - 1, rows_of(k)], rs_r.at[d, st - 1, k])
                    others = [rrs.at[d, st - 1]]
                gate, val = summed(o, k, others)
                if k == 0:
                    srs[d, st, pl.ds(0, gate_rows), :] = gate.astype(BF)
                srs[d, st, pl.ds(gate_rows + k * vr, vr), :] = val.astype(BF)
                rs_send(d, st, k)
                started.append((d, st, k))
            if st > 0:
                some_weights(-(-2 * NY // (NG * (hop - 1))) if hop > 1 else 2 * NY)
        pairs_up_to(NY)
        if st == 0:
            n = out_sh.shape[0]
            arrived(shp.at[pl.ds(n, (blocks - 1) * n)], sh_r)
            own = shp[pl.ds(pl.multiple_of(ep * n, n), n), :].astype(F32)
            out_sh[...] = lax.fori_loop(
                1, blocks, lambda r, acc: acc + shr[r].astype(F32), own
            )
    some_weights(2 * NY)
    stores = [
        pltpu.make_async_copy(dgu.at[pl.ds(0, hid)], out_wg.at[0], osem.at[0]),
        pltpu.make_async_copy(dgu.at[pl.ds(hid, hid)], out_wu.at[0], osem.at[1]),
        pltpu.make_async_copy(ddn, out_wd.at[0], osem.at[2]),
    ]
    for store in stores:
        store.start()

    need(0)
    gates = None
    for k in range(NG):
        for d in range(2):
            arrived(rrs.at[d, hop - 1, rows_of(k)], rs_r.at[d, hop - 1, k])
        gate, val = summed(0, k, [rrs.at[0, hop - 1], rrs.at[1, hop - 1]])
        if k == 0:
            gates = gate
        at = (k * size // gate_rows) * 128
        fin[k, pl.ds(0, gate_rows), :] = jnp.concatenate(
            [gates[:, at : at + 128], jnp.zeros((gate_rows, feats - 128), F32)], axis=1
        ).astype(BF)
        fin[k, pl.ds(gate_rows, vr), :] = val.astype(BF)
        fin[k, pl.ds(gate_rows + vr, br - gate_rows - vr), :] = jnp.zeros(
            (br - gate_rows - vr, feats), BF
        )
        sb[pl.ds(k * br, br), :] = dot(spread[k % 2], fin[k]).astype(BF)

        def home(r, carry, k=k):
            rows = pl.ds(pl.multiple_of(r * ROWS, ROWS), ROWS)
            send(sb.at[rows], rb.at[rows], rb_s, rb_r.at[k], (behind(r), tp))
            return carry

        lax.fori_loop(max(1, k * size), (k + 1) * size, home, 0)
    rb[pl.ds(0, ROWS), :] = sb[pl.ds(0, ROWS), :]

    after = (
        lax.broadcasted_iota(jnp.int32, (n_tok, n_tok), 1)
        < lax.broadcasted_iota(jnp.int32, (n_tok, n_tok), 0)
    ).astype(BF)
    names_t = lax.broadcasted_iota(jnp.int32, (n_tok, blocks), 1)
    cols_e = [routes[:, k : k + 1] for k in range(2)]
    hot_t = [(names_t == e).astype(F32) for e in cols_e]
    seen_t = dot(after, (hot_t[0] + hot_t[1]).astype(BF))
    position = [jnp.sum(hot_t[k] * seen_t, axis=1, keepdims=True) for k in range(2)]
    block = [rank_of(e) * ROWS for e in cols_e]
    slots_t = lax.broadcasted_iota(jnp.int32, (n_tok, blocks * ROWS), 1).astype(F32)
    picks = [(slots_t == block[k] + position[k]).astype(F32) for k in range(2)]
    gate_at = [(slots_t == block[k] + float(cap)).astype(BF) for k in range(2)]
    lanes = lax.broadcasted_iota(jnp.int32, (n_tok, feats), 1).astype(F32)

    for k in range(NG):
        lo = ROWS if k == 0 else 0
        arrived(rb.at[pl.ds(k * br + lo, br - lo)], rb_r.at[k])
    rows_back = rb[...]
    out_tok[...] = dot((picks[0] + picks[1]).astype(BF), rows_back).astype(BF)
    parts = []
    for k in range(2):
        found = jnp.where(lanes == position[k], dot(gate_at[k], rows_back), 0.0)
        parts.append(jnp.sum(found, axis=1, keepdims=True) / gw[:, k : k + 1])
    out_gate[...] = jnp.concatenate(parts, axis=1)

    arrived(sx.at[pl.ds(ROWS, (blocks - 1) * ROWS)], a2a_s.at[0])
    arrived(sg.at[pl.ds(ROWS, (blocks - 1) * ROWS)], a2a_s.at[1])
    arrived(shp.at[pl.ds(out_sh.shape[0], (blocks - 1) * out_sh.shape[0])], sh_s)
    for a in range(2):
        for d in range(2):
            for h in range(hop):
                n = total if h < hop - 1 else half
                arrived(xg.at[a, 0, pl.ds(0, n)], ag_s.at[a, d, h])
        arrived(xg.at[a, pl.ds(0, NY)], sib_s.at[a])
    arrived(ps, pair_s)
    for d, st, k in started:
        arrived(srs.at[d, st, rows_of(k)], rs_s.at[d, st, k])
    arrived(sb.at[pl.ds(ROWS, (blocks - 1) * ROWS)], rb_s)
    for store in stores:
        store.wait()


def shards(tokens, cotangent, routes, gate_weight, w_gate, w_up, w_down, shared_hidden):
    n_tok, feats = tokens.shape
    blocks = NZ * NX
    cap = 3 * n_tok * routes.shape[1] // (2 * blocks)
    total, size, hop = blocks * cap, blocks // NG, NY // 2
    hid, width = w_gate.shape[1:]
    chunk = total + blocks // 2
    n_sh = shared_hidden.shape[1] // blocks
    shared = jnp.dot(shared_hidden.T, cotangent, preferred_element_type=F32).astype(BF)
    dma = pltpu.SemaphoreType.DMA
    vm = pl.BlockSpec(memory_space=pltpu.VMEM)
    hbm = pl.BlockSpec(memory_space=pl.ANY)
    sent = (blocks * ROWS, feats)
    weight_out = jax.ShapeDtypeStruct((1, hid, width), F32)
    return pl.pallas_call(
        lambda *refs: layer(cap, *refs),
        out_shape=(
            jax.ShapeDtypeStruct((n_tok, feats), BF),
            jax.ShapeDtypeStruct((n_tok, 2), F32),
            weight_out,
            weight_out,
            weight_out,
            jax.ShapeDtypeStruct((n_sh, feats), F32),
        ),
        in_specs=[vm] * 11 + [hbm] * 3,
        out_specs=(vm, vm, hbm, hbm, hbm, vm),
        scratch_shapes=[
            pltpu.VMEM((2 * hid, width), BF),
            pltpu.VMEM((hid, width), BF),
            pltpu.VMEM(sent, BF),
            pltpu.VMEM(sent, BF),
            pltpu.VMEM(sent, BF),
            pltpu.VMEM(sent, BF),
            pltpu.VMEM((2, 2 * NY, total, feats), BF),
            pltpu.VMEM((blocks, n_sh, feats), BF),
            pltpu.VMEM((2 * hid, total), F32),
            pltpu.VMEM((hid, total), F32),
            pltpu.VMEM((2 * hid, total), BF),
            pltpu.VMEM((total, 2 * hid), BF),
            pltpu.VMEM((hid, total), BF),
            pltpu.VMEM((blocks // 2, feats), F32),
            pltpu.VMEM((NY, chunk, feats), BF),
            pltpu.VMEM((NY, chunk, feats), BF),
            pltpu.VMEM((2, hop, chunk, feats), BF),
            pltpu.VMEM((2, hop, chunk, feats), BF),
            pltpu.VMEM((NG, size * ROWS, feats), BF),
            pltpu.VMEM(sent, BF),
            pltpu.VMEM(sent, BF),
            pltpu.VMEM((2 * hid, width), F32),
            pltpu.VMEM((hid, width), F32),
            dma((3,)),
            dma((3,)),
            dma((2,)),
            dma((2, NG)),
            dma((2, 2, hop)),
            dma((2, 2, hop, 2)),
            dma((2,)),
            dma((2, NY, 2)),
            dma,
            dma,
            dma,
            dma((NY,)),
            dma((2, hop, NG)),
            dma((2, hop, NG)),
            dma,
            dma((NG,)),
        ],
        compiler_params=pltpu.CompilerParams(
            collective_id=0, has_side_effects=True, vmem_limit_bytes=56 * 1024 * 1024
        ),
    )(
        tokens, cotangent, routes, routes.T, gate_weight, gate_weight.T, shared,
        *constants(blocks, cap), w_gate, w_up, w_down,
    )


def solution(mesh):
    placed = (
        P("ep", "tp"),
        P("ep", "tp"),
        P("ep", None),
        P("ep", None),
        P("ep", "tp", None),
        P("ep", "tp", None),
        P("ep", "tp", None),
        P("ep", None),
    )
    return jax.shard_map(
        shards,
        mesh=mesh,
        in_specs=placed,
        out_specs=(
            P("ep", "tp"),
            P("ep", None),
            P("ep", "tp", None),
            P("ep", "tp", None),
            P("ep", "tp", None),
            P("ep", "tp"),
        ),
        check_vma=False,
    )
```

```python
import jax
import jax.numpy as jnp
import numpy as np
from jax import lax
from jax.experimental import pallas as pl
from jax.experimental.pallas import tpu as pltpu
from jax.sharding import PartitionSpec as P

MESH = pl.DeviceIdType.MESH
NZ, NX, NY = 8, 4, 8
NG = 4
ROWS = 16
BF = jnp.bfloat16
F32 = jnp.float32


def constants(blocks, cap):
    size = blocks // NG
    packed, gate_rows = size * cap, blocks // 2
    pack = np.zeros((packed, size * ROWS), np.float32)
    for q in range(size):
        for p in range(cap):
            pack[q * cap + p, q * ROWS + p] = 1
    spread = np.zeros((2, size * ROWS, size * ROWS), np.float32)
    for par in range(2):
        for q in range(size):
            for p in range(cap):
                spread[par, q * ROWS + p, gate_rows + q * cap + p] = 1
            spread[par, q * ROWS + cap, par * size + q] = 1
    total = blocks * cap
    owner = np.zeros((blocks, total), np.float32)
    place = np.zeros((total, 128), np.float32)
    for s in range(total):
        owner[s // cap, s] = 1
        place[s, s % cap] = 1
    return [jnp.asarray(a, BF) for a in (pack, spread)] + [
        jnp.asarray(owner, F32), jnp.asarray(place, BF)
    ]


def layer(cap, *refs):
    (tok_in, cot_in, routes_in, gw_in, pack_in, spread_in) = refs[:6]
    (owner_in, place_in, shid_in, wg, wu, wd) = refs[6:12]
    (out_tok, out_gate, out_wg, out_wu, out_wd, out_sh) = refs[12:18]
    (w2, wdn, sx, sg, rx, rg, xg, shr, pre, back, gt, gn, ht, tile, ps, pr, srs, rrs) = refs[18:36]
    (fin, sb, rb, shp, shid, pack, spread, owner, place, tok, cot, routes_t, gw_t) = refs[36:49]
    (wsem, a2a_s, a2a_r, ag_s, ag_r, sib_s, sib_r, sh_s, sh_r) = refs[49:58]
    (pair_s, pair_r, rs_s, rs_r, rb_s, rb_r) = refs[58:]

    n_tok, feats = tok.shape
    blocks = NZ * NX
    size = blocks // NG
    vr, br, gate_rows = size * cap, size * ROWS, blocks // 2
    total = blocks * cap
    hop = NY // 2
    half = total // 2
    hid = wdn.shape[0]
    ep, tp = lax.axis_index("ep"), lax.axis_index("tp")
    z, x, y, c = ep // NX, ep % NX, tp // 2, tp % 2
    sibling = y * 2 + 1 - c

    def offset(r):
        q = r // NX
        odd = q % 2
        return (odd * ((q + 1) // 2) + (1 - odd) * (NZ - q // 2)) % NZ, r % NX

    def ahead(r):
        dz, dx = offset(r)
        return ((z + dz) % NZ) * NX + (x + dx) % NX

    def behind(r):
        dz, dx = offset(r)
        return ((z - dz + NZ) % NZ) * NX + (x - dx + NX) % NX

    def own_col(o):
        return ((y + o) % NY) * 2 + c

    def sib_col(o):
        return ((y + o) % NY) * 2 + 1 - c

    def arrived(ref, sem):
        pltpu.make_async_remote_copy(
            src_ref=ref, dst_ref=ref, send_sem=sem, recv_sem=sem,
            device_id=(ep, sibling), device_id_type=MESH,
        ).wait_recv()

    def send(src, dst, s_sem, r_sem, device):
        pltpu.make_async_remote_copy(
            src_ref=src, dst_ref=dst, send_sem=s_sem, recv_sem=r_sem,
            device_id=device, device_id_type=MESH,
        ).start()

    def dot(a, b):
        return jnp.dot(a, b, preferred_element_type=F32)

    def dot_nt(a, b):
        return lax.dot_general(a, b, (((1,), (1,)), ((), ())), preferred_element_type=F32)

    firsts = [
        pltpu.make_async_copy(src, dst, wsem.at[i])
        for i, (src, dst) in enumerate(
            ((routes_in, routes_t), (gw_in, gw_t), (tok_in, tok), (cot_in, cot), (pack_in, pack))
        )
    ]
    for load in firsts:
        load.start()

    barrier = pltpu.get_barrier_semaphore()

    def greet(r, carry):
        pl.semaphore_signal(barrier, inc=1, device_id=(ahead(r), tp), device_id_type=MESH)
        return carry

    lax.fori_loop(1, blocks, greet, 0)
    for peer in (((y + 1) % NY) * 2 + c, ((y + NY - 1) % NY) * 2 + c, sibling):
        pl.semaphore_signal(barrier, inc=1, device_id=(ep, peer), device_id_type=MESH)

    loads = [
        pltpu.make_async_copy(wg.at[0], w2.at[pl.ds(0, hid)], wsem.at[5]),
        pltpu.make_async_copy(wu.at[0], w2.at[pl.ds(hid, hid)], wsem.at[6]),
        pltpu.make_async_copy(wd.at[0], wdn, wsem.at[7]),
        pltpu.make_async_copy(owner_in, owner, wsem.at[8]),
        pltpu.make_async_copy(place_in, place, wsem.at[9]),
        pltpu.make_async_copy(spread_in, spread, wsem.at[10]),
    ]
    load_sh = pltpu.make_async_copy(shid_in, shid, wsem.at[11])
    for load in [load_sh, *loads]:
        load.start()

    def rank_of(e):
        ez, ex = e // NX if NX & (NX - 1) else e >> (NX.bit_length() - 1), e & (NX - 1)
        dz, dx = (ez - z + NZ) & (NZ - 1), (ex - x + NX) & (NX - 1)
        q = jnp.where(dz <= NZ // 2, jnp.maximum(2 * dz - 1, 0), 2 * (NZ - dz))
        return (q * NX + dx).astype(F32)

    before = (
        lax.broadcasted_iota(jnp.int32, (n_tok, n_tok), 0)
        < lax.broadcasted_iota(jnp.int32, (n_tok, n_tok), 1)
    ).astype(F32)
    names = lax.broadcasted_iota(jnp.int32, (blocks, n_tok), 0)
    for load in firsts:
        load.wait()
    rows_e = [routes_t[k : k + 1, :] for k in range(2)]
    hot = [(names == e).astype(F32) for e in rows_e]
    seen = dot((hot[0] + hot[1]).astype(BF), before.astype(BF))
    block_rows = [rank_of(e) * ROWS for e in rows_e]
    place_rows = [jnp.sum(hot[k] * seen, axis=0, keepdims=True) for k in range(2)]
    slot_rows = [block_rows[k] + place_rows[k] for k in range(2)]
    slots = lax.broadcasted_iota(jnp.int32, (blocks * ROWS, n_tok), 0).astype(F32)
    chosen = [(slots == d).astype(F32) for d in slot_rows]
    weight = jnp.sum(
        chosen[0] * gw_t[0:1, :] + chosen[1] * gw_t[1:2, :], axis=1, keepdims=True
    )
    table = (chosen[0] + chosen[1]).astype(BF)
    sx[...] = dot(table, tok[...]).astype(BF)
    sg[...] = (dot(table, cot[...]) * weight).astype(BF)
    rx[pl.ds(0, ROWS), :] = sx[pl.ds(0, ROWS), :]
    rg[pl.ds(0, ROWS), :] = sg[pl.ds(0, ROWS), :]

    pl.semaphore_wait(barrier, blocks - 1 + 3)

    for a, (src, dst) in enumerate(((sx, rx), (sg, rg))):
        for g in range(NG):

            def to_expert(r, carry, a=a, src=src, dst=dst, g=g):
                rows = pl.ds(pl.multiple_of(r * ROWS, ROWS), ROWS)
                send(src.at[rows], dst.at[rows], a2a_s.at[a], a2a_r.at[a, g], (ahead(r), tp))
                return carry

            lax.fori_loop(max(1, g * size), (g + 1) * size, to_expert, 0)

    def share(r, carry):
        e = ahead(r)
        n = out_sh.shape[0]
        rows = pl.ds(pl.multiple_of(e * n, n), n)
        send(shp.at[rows], shr.at[r], sh_s, sh_r, (e, tp))
        return carry

    def ring(a, way, h, k):
        d = 0 if way > 0 else 1
        part = xg.at[a, own_col(NY - h * way), pl.ds(k * half, half)]
        send(part, part, ag_s.at[a, d, h], ag_r.at[a, d, h, k], (ep, ((y + way + NY) % NY) * 2 + c))

    def to_sibling(a, o, k):
        part = xg.at[a, own_col(o), pl.ds(k * half, half)]
        send(part, part, sib_s.at[a], sib_r.at[a, o, k], (ep, sibling))

    load_sh.wait()
    terms = lax.dot_general(
        shid[...], cot[...], (((0,), (0,)), ((), ())), preferred_element_type=F32
    )
    shp[...] = terms.astype(BF)

    for a, dst in enumerate((rx, rg)):
        for g in range(NG):
            lo = ROWS if g == 0 else 0
            arrived(dst.at[pl.ds(g * br + lo, br - lo)], a2a_r.at[a, g])
            got = dot(pack[...], dst[pl.ds(g * br, br), :])
            xg[a, own_col(0), pl.ds(g * vr, vr), :] = got.astype(BF)
            if g % 2 == 1:
                k = g // 2
                for way in (1, -1):
                    if hop > 1 or k == (0 if way > 0 else 1):
                        ring(a, way, 0, k)
                to_sibling(a, 0, k)
        if a == 1:
            lax.fori_loop(1, blocks, share, 0)

    for load in loads:
        load.wait()

    def forward(a, o, first=False):
        for k in range(2):
            arrived(xg.at[a, sib_col(o), pl.ds(k * half, half)], sib_r.at[a, o, k])
        acc, w = (pre, w2) if a == 0 else (back, wdn)
        part = None
        for j in (own_col(o), sib_col(o)):
            cols = pl.ds(pl.multiple_of(j * feats, feats), feats)
            term = dot_nt(w[:, cols], xg[a, j])
            part = term if part is None else part + term
        acc[...] = part if first else acc[...] + part

    for h in range(1, hop + 1):
        for a in range(2):
            for k in range(2):
                for d, way in enumerate((1, -1)):
                    if h == hop and k != d:
                        continue
                    o = (NY - h * way) % NY
                    part = xg.at[a, own_col(o), pl.ds(k * half, half)]
                    arrived(part, ag_r.at[a, d, h - 1, k])
                    if h < hop - 1 or (h == hop - 1 and k == d):
                        ring(a, way, h, k)
                    to_sibling(a, o, k)
        for a in range(2):
            if h == 1:
                forward(a, 0, first=True)
            else:
                forward(a, h - 1)
                forward(a, NY - h + 1)
    for a in range(2):
        forward(a, hop)

    s, u, b = pre[pl.ds(0, hid), :], pre[pl.ds(hid, hid), :], back[...]
    sig = 1.0 / (1.0 + jnp.exp(-s))
    silu = s * sig
    hidden = (silu * u).astype(BF)
    ht[...] = hidden
    grad_gate = b * u * sig * (1.0 + s * (1.0 - sig))
    grad_up = b * silu
    both = jnp.concatenate([grad_gate, grad_up], axis=0)
    gt[...] = both.astype(BF)
    gn[...] = both.T.astype(BF)
    gate_row = jnp.sum(hidden.astype(F32) * b, axis=0, keepdims=True)
    by_block = dot((owner[...] * gate_row).astype(BF), place[...])
    tile[...] = jnp.concatenate([by_block[:gate_rows], by_block[gate_rows:]], axis=1)

    def pair(o):
        cols = pl.ds(pl.multiple_of(sib_col(o) * feats, feats), feats)
        ps[o, pl.ds(0, gate_rows), :] = tile[...].astype(BF)
        ps[o, pl.ds(gate_rows, total), :] = dot(gn[...], w2[:, cols]).astype(BF)
        send(ps.at[o], pr.at[o], pair_s, pair_r.at[o], (ep, sibling))

    def rows_of(k):
        return pl.ds(0, gate_rows + vr) if k == 0 else pl.ds(gate_rows + k * vr, vr)

    def summed(o, k, others):
        cols = pl.ds(pl.multiple_of(own_col(o) * feats, feats), feats)
        mine = dot(gn[pl.ds(k * vr, vr), :], w2[:, cols])
        rest = pr[o, rows_of(k), :].astype(F32)
        for ref in others:
            rest = rest + ref[rows_of(k), :].astype(F32)
        if k > 0:
            return None, rest + mine
        return rest[:gate_rows] + tile[...], rest[gate_rows:] + mine

    def weights(j):
        cols = pl.ds(j * feats, feats)
        grads = dot(gt[...], xg[0, j])
        out_wg[0, :, cols] = grads[:hid]
        out_wu[0, :, cols] = grads[hid:]
        out_wd[0, :, cols] = dot(ht[...], xg[1, j])

    def rs_send(d, st, k):
        way = 1 - 2 * d
        part = pl.ds(*((0, gate_rows + vr) if k == 0 else (gate_rows + k * vr, vr)))
        send(
            srs.at[d, st, part], rrs.at[d, st, part], rs_s.at[d, st, k], rs_r.at[d, st, k],
            (ep, ((y + way + NY) % NY) * 2 + c),
        )

    started, todo = [], list(range(2 * NY))

    def some_weights(n):
        for _ in range(n):
            if todo:
                weights(todo.pop(0))

    pending = [hop] + [o for i in range(hop - 1, 0, -1) for o in (i, NY - i)] + [0]
    done = []

    def pairs_up_to(n):
        while len(done) < n:
            pair(pending[len(done)])
            done.append(1)

    ready = []

    def need(o):
        if o not in ready:
            arrived(pr.at[o], pair_r.at[o])
            ready.append(o)

    pairs_up_to(3)
    for st in range(hop):
        for k in range(NG):
            for d in range(2):
                mine = k // (NG // 2) == d
                if st == 0 and not mine:
                    continue
                way = 1 - 2 * d
                o = (way * (hop - st)) % NY
                need(o)
                others = []
                if st > 1 or (st == 1 and mine):
                    arrived(rrs.at[d, st - 1, rows_of(k)], rs_r.at[d, st - 1, k])
                    others = [rrs.at[d, st - 1]]
                gate, val = summed(o, k, others)
                if k == 0:
                    srs[d, st, pl.ds(0, gate_rows), :] = gate.astype(BF)
                srs[d, st, pl.ds(gate_rows + k * vr, vr), :] = val.astype(BF)
                rs_send(d, st, k)
                started.append((d, st, k))
            if st > 0:
                some_weights(-(-2 * NY // (NG * (hop - 1))) if hop > 1 else 2 * NY)
        pairs_up_to(NY)
        if st == 0:
            n = out_sh.shape[0]
            arrived(shp.at[pl.ds(n, (blocks - 1) * n)], sh_r)
            own = shp[pl.ds(pl.multiple_of(ep * n, n), n), :].astype(F32)
            out_sh[...] = lax.fori_loop(
                1, blocks, lambda r, acc: acc + shr[r].astype(F32), own
            )
    some_weights(2 * NY)

    need(0)
    gates = None
    for k in range(NG):
        for d in range(2):
            arrived(rrs.at[d, hop - 1, rows_of(k)], rs_r.at[d, hop - 1, k])
        gate, val = summed(0, k, [rrs.at[0, hop - 1], rrs.at[1, hop - 1]])
        if k == 0:
            gates = gate
        at = (k * size // gate_rows) * 128
        fin[k, pl.ds(0, gate_rows), :] = jnp.concatenate(
            [gates[:, at : at + 128], jnp.zeros((gate_rows, feats - 128), F32)], axis=1
        ).astype(BF)
        fin[k, pl.ds(gate_rows, vr), :] = val.astype(BF)
        fin[k, pl.ds(gate_rows + vr, br - gate_rows - vr), :] = jnp.zeros(
            (br - gate_rows - vr, feats), BF
        )
        sb[pl.ds(k * br, br), :] = dot(spread[k % 2], fin[k]).astype(BF)

        def home(r, carry, k=k):
            rows = pl.ds(pl.multiple_of(r * ROWS, ROWS), ROWS)
            send(sb.at[rows], rb.at[rows], rb_s, rb_r.at[k], (behind(r), tp))
            return carry

        lax.fori_loop(max(1, k * size), (k + 1) * size, home, 0)
    rb[pl.ds(0, ROWS), :] = sb[pl.ds(0, ROWS), :]

    ones = lax.broadcasted_iota(jnp.int32, (n_tok, n_tok), 0) == lax.broadcasted_iota(
        jnp.int32, (n_tok, n_tok), 1
    )

    def to_col(row):
        return jnp.sum(jnp.where(ones, row, 0.0), axis=1, keepdims=True)

    def to_row(col):
        return jnp.sum(jnp.where(ones, col, 0.0), axis=0, keepdims=True)

    position = [to_col(r) for r in place_rows]
    block = [to_col(r) for r in block_rows]
    slots_t = lax.broadcasted_iota(jnp.int32, (n_tok, blocks * ROWS), 1).astype(F32)
    picks = [(slots_t == block[k] + position[k]).astype(F32) for k in range(2)]
    gate_at = [(slots_t == block[k] + float(cap)).astype(BF) for k in range(2)]
    lanes = lax.broadcasted_iota(jnp.int32, (n_tok, feats), 1).astype(F32)

    for k in range(NG):
        lo = ROWS if k == 0 else 0
        arrived(rb.at[pl.ds(k * br + lo, br - lo)], rb_r.at[k])
    rows_back = rb[...]
    out_tok[...] = dot((picks[0] + picks[1]).astype(BF), rows_back).astype(BF)
    parts = []
    for k in range(2):
        found = jnp.where(lanes == position[k], dot(gate_at[k], rows_back), 0.0)
        parts.append(to_row(jnp.sum(found, axis=1, keepdims=True)))
    out_gate[...] = jnp.concatenate(parts, axis=0) / gw_t[...]

    arrived(sx.at[pl.ds(ROWS, (blocks - 1) * ROWS)], a2a_s.at[0])
    arrived(sg.at[pl.ds(ROWS, (blocks - 1) * ROWS)], a2a_s.at[1])
    arrived(shp.at[pl.ds(out_sh.shape[0], (blocks - 1) * out_sh.shape[0])], sh_s)
    for a in range(2):
        for d in range(2):
            for h in range(hop):
                n = total if h < hop - 1 else half
                arrived(xg.at[a, 0, pl.ds(0, n)], ag_s.at[a, d, h])
        arrived(xg.at[a, pl.ds(0, NY)], sib_s.at[a])
    arrived(ps, pair_s)
    for d, st, k in started:
        arrived(srs.at[d, st, rows_of(k)], rs_s.at[d, st, k])
    arrived(sb.at[pl.ds(ROWS, (blocks - 1) * ROWS)], rb_s)


def hand_out(*refs):
    n = len(refs) // 2
    moves = [pltpu.make_async_copy(refs[i], refs[n + i], refs[-1].at[i]) for i in range(n)]
    for move in moves:
        move.start()
    for move in moves:
        move.wait()


def shards(tokens, cotangent, routes, gate_weight, w_gate, w_up, w_down, shared_hidden):
    n_tok, feats = tokens.shape
    blocks = NZ * NX
    cap = 3 * n_tok * routes.shape[1] // (2 * blocks)
    total, size, hop = blocks * cap, blocks // NG, NY // 2
    hid, width = w_gate.shape[1:]
    chunk = total + blocks // 2
    n_sh = shared_hidden.shape[1] // blocks
    consts = constants(blocks, cap)
    dma = pltpu.SemaphoreType.DMA
    vm = pl.BlockSpec(memory_space=pltpu.VMEM)
    hbm = pl.BlockSpec(memory_space=pltpu.HBM)
    sent = (blocks * ROWS, feats)
    weight_out = jax.ShapeDtypeStruct((1, hid, width), F32)
    out_shape = (
        jax.ShapeDtypeStruct((n_tok, feats), BF),
        jax.ShapeDtypeStruct((2, n_tok), F32),
        weight_out,
        weight_out,
        weight_out,
        jax.ShapeDtypeStruct((n_sh, feats), F32),
    )
    outs = pl.pallas_call(
        lambda *refs: layer(cap, *refs),
        out_shape=out_shape,
        in_specs=[hbm] * 12,
        out_specs=(vm,) * 6,
        scratch_shapes=[
            pltpu.VMEM((2 * hid, width), BF),
            pltpu.VMEM((hid, width), BF),
            pltpu.VMEM(sent, BF),
            pltpu.VMEM(sent, BF),
            pltpu.VMEM(sent, BF),
            pltpu.VMEM(sent, BF),
            pltpu.VMEM((2, 2 * NY, total, feats), BF),
            pltpu.VMEM((blocks, n_sh, feats), BF),
            pltpu.VMEM((2 * hid, total), F32),
            pltpu.VMEM((hid, total), F32),
            pltpu.VMEM((2 * hid, total), BF),
            pltpu.VMEM((total, 2 * hid), BF),
            pltpu.VMEM((hid, total), BF),
            pltpu.VMEM((blocks // 2, feats), F32),
            pltpu.VMEM((NY, chunk, feats), BF),
            pltpu.VMEM((NY, chunk, feats), BF),
            pltpu.VMEM((2, hop, chunk, feats), BF),
            pltpu.VMEM((2, hop, chunk, feats), BF),
            pltpu.VMEM((NG, size * ROWS, feats), BF),
            pltpu.VMEM(sent, BF),
            pltpu.VMEM(sent, BF),
            pltpu.VMEM((blocks * n_sh, feats), BF),
            pltpu.VMEM(shared_hidden.shape, BF),
            *(pltpu.VMEM(c.shape, c.dtype) for c in consts),
            pltpu.VMEM((n_tok, feats), BF),
            pltpu.VMEM((n_tok, feats), BF),
            pltpu.VMEM((2, n_tok), jnp.int32),
            pltpu.VMEM((2, n_tok), F32),
            dma((12,)),
            dma((2,)),
            dma((2, NG)),
            dma((2, 2, hop)),
            dma((2, 2, hop, 2)),
            dma((2,)),
            dma((2, NY, 2)),
            dma,
            dma,
            dma,
            dma((NY,)),
            dma((2, hop, NG)),
            dma((2, hop, NG)),
            dma,
            dma((NG,)),
        ],
        compiler_params=pltpu.CompilerParams(
            collective_id=0, has_side_effects=True, vmem_limit_bytes=28 * 1024 * 1024
        ),
    )(
        *(
            pltpu.with_memory_space_constraint(a, pltpu.HBM)
            for a in (
                tokens, cotangent, routes.T, gate_weight.T, *consts, shared_hidden,
                w_gate, w_up, w_down,
            )
        )
    )
    outs = pl.pallas_call(
        hand_out,
        out_shape=out_shape,
        in_specs=[vm] * 6,
        out_specs=(hbm,) * 6,
        scratch_shapes=[dma((6,))],
    )(*(pltpu.with_memory_space_constraint(a, pltpu.VMEM) for a in outs))
    return (outs[0], outs[1].T, *outs[2:])


def solution(mesh):
    placed = (
        P("ep", "tp"),
        P("ep", "tp"),
        P("ep", None),
        P("ep", None),
        P("ep", "tp", None),
        P("ep", "tp", None),
        P("ep", "tp", None),
        P("ep", None),
    )
    return jax.shard_map(
        shards,
        mesh=mesh,
        in_specs=placed,
        out_specs=(
            P("ep", "tp"),
            P("ep", None),
            P("ep", "tp", None),
            P("ep", "tp", None),
            P("ep", "tp", None),
            P("ep", "tp"),
        ),
        check_vma=False,
    )
```
